256 devices in a mesh: ep: 64 (over z, x, core), tp: 4 (over y).
Axes of the slice: x: 4, y: 4, z: 8, core: 2. Of those that a mesh axis runs over, the one named last changes fastest.
Arguments:
- conv_input: bfloat16 [65536, 2048], P('ep', 'tp'), may hold values from -6 to 6
- conv_kernel: bfloat16 [31, 2048], P(None, 'tp'), may hold values from -2 to 2
- norm_gain: float32 [2048], P('tp'), may hold values from 0.1 to 1.9
- norm_shift: float32 [2048], P('tp'), may hold values from -3 to 3
- conv_proj: bfloat16 [2048, 2048], P('tp'), may hold values from -0.125 to 0.125
- moe_input: bfloat16 [16384, 2048], P(('ep', 'tp')), may hold values from -6 to 6
- moe_gain: float32 [2048], replicated, may hold values from 0.1 to 1.9
- routes: int32 [16384, 2], P('ep'), may hold values from 0 to 63, all different within a row; in each aligned block of 256 rows (0 to 255, 256 to 511, ...) at most 16 rows name the same one
- route_weights: float32 [16384, 2], P('ep'), may hold values from 0.2 to 1
- gate_proj: bfloat16 [64, 2048, 2048], P('ep', None, 'tp'), may hold values from -0.125 to 0.125
- up_proj: bfloat16 [64, 2048, 2048], P('ep', None, 'tp'), may hold values from -0.125 to 0.125
- down_proj: bfloat16 [64, 2048, 2048], P('ep', 'tp'), may hold values from -0.125 to 0.125
Outputs:
- conv_out: bfloat16 [65536, 2048], P(('ep', 'tp'))
- moe_out: bfloat16 [16384, 2048], P(('ep', 'tp'))
The draws below stay inside these ranges and needn't reach their ends.
Inputs may be any that keep to these rules, and one draw needn't show every extreme that they name: `routes`: each row names 2 different experts. In each aligned block of 256 rows no expert is named by more than 16 rows, and in some blocks an expert is named by exactly 16 rows.
All inputs are finite; a program needn't handle non-finite values.
Results may differ from the reference program's by a relative error of at most 0.012.
Values may be sent and summed in bfloat16 or wider, within the bound.
No kernel may reach another device: no remote copies, remote signals or barrier semaphores. Data moves between devices by JAX's collectives and lax.ppermute only.
A program may use at most 128 MiB of HBM per device.

```python
import math
import jax
import jax.numpy as jnp
import numpy as np
from jax import lax

D = 2048
FE = 2048
CONV_WIDTH = 31
TOPK = 2
TOK_DEV = 64
EXPERTS = 64
CAPG = 16
CONV_TOKENS = 65536
MOE_TOKENS = 16384
N_EP = 64
N_TP = 4


def draw_conv_kernel(key, part):
    first_key, second_key = jax.random.split(jax.random.fold_in(key, 11))
    factors = jax.random.permutation(first_key, jnp.array([0.5, 0.9, 1.6, 2.6], jnp.float32))
    channel_block = jnp.arange(D, dtype=jnp.int32) * 4 // D
    column_scale = factors[channel_block] / math.sqrt(CONV_WIDTH)
    base = jnp.clip(jax.random.normal(second_key, (CONV_WIDTH, D), jnp.float32), -4.0, 4.0)
    return (base * column_scale[None, :]).astype(jnp.bfloat16)


def shard_levels(stream_key, extent, cuts, least, top_value):
    def one(axis_at, parts):
        heights = jax.random.uniform(jax.random.fold_in(jax.random.fold_in(stream_key, 6), axis_at), (parts,), jnp.float32, least / len(cuts), top_value / len(cuts))
        return jnp.repeat(jnp.exp(heights), extent[axis_at] // parts).reshape((-1,) + (1,) * (len(extent) - axis_at - 1))

    factor_of = one(*cuts[0])
    for cut in cuts[1:]:
        factor_of = factor_of * one(*cut)
    return factor_of


def assign_block(own_key, own, number, rows, number_of, top, most, slope):
    ranking = jax.random.permutation(own_key, number_of)
    packed, usual = load_shares(number_of, rows * top, most, slope, True), load_shares(number_of, rows * top, most, slope, False)
    places = jnp.arange(number_of)

    def named(sizes, offset_by):
        used = int((sizes > 0).sum())
        fixed = max(1, used // 4)
        moved = fixed + (places - fixed + offset_by * (used - fixed)) % max(1, number_of - fixed)
        return jnp.zeros((number_of,), jnp.int32).at[ranking[jnp.where(places < fixed, places, moved)]].set(jnp.asarray(sizes, jnp.int32))

    sizes = jnp.where(number % 4 == 0, named(packed, number // 4), named(usual, number - number // 4 - 1))
    mixed = jax.random.permutation(jax.random.fold_in(own, 3), number_of)
    giver, taker = mixed[0:number_of // 2 * 2:2], mixed[1:number_of // 2 * 2:2]
    slack = jnp.minimum(sizes[giver] - 1, most - sizes[taker]) // 2
    slack = jnp.where((giver == ranking[0]) | (taker == ranking[0]) | (sizes[taker] == 0), 0, jnp.maximum(slack, 0))
    moved = jax.random.randint(jax.random.fold_in(own, 4), (number_of // 2,), 0, 1 << 20) % (slack + 1)
    sizes = sizes.at[giver].add(-moved).at[taker].add(moved)
    labels = jnp.searchsorted(jnp.cumsum(sizes), jnp.arange(rows * top), side="right").astype(jnp.int32)
    listing = labels.reshape(top, rows).T
    listing = listing[jax.random.permutation(jax.random.fold_in(own, 1), rows)]
    offset_by = jax.random.randint(jax.random.fold_in(own, 2), (rows, 1), 0, top)
    return jnp.take_along_axis(listing, (jnp.arange(top)[None, :] + offset_by) % top, axis=1)


def load_shares(amount, total, most, slope, full):
    portions = [(1 << 20) // math.isqrt(standing ** slope) + 1 for standing in range(1, amount + 1)]
    largest = most if full else min(most, max(-(-total // amount), total * portions[0] // sum(portions)))
    least = 1 if total - largest >= amount - 1 else 0
    counts, rest = [largest] + [least] * (amount - 1), total - largest - least * (amount - 1)
    while rest > 0:
        candidates = [i for i in range(1, amount) if counts[i] < largest] or [i for i in range(1, amount) if counts[i] < most]
        whole, left = sum([portions[i] for i in candidates]), rest
        for i in candidates:
            more = min(most - counts[i], max(1, left * portions[i] // whole), rest)
            counts[i] = counts[i] + more
            rest = rest - more
    return np.array(counts)


def noise(stream_key, extent, scale, limit, cuts=(), held_as=jnp.bfloat16):
    gain = shard_levels(stream_key, extent, cuts, -0.22, 0.18) if cuts else 1.0
    entries = jax.random.normal(stream_key, extent, jnp.float32) * scale * gain
    return jnp.minimum(jnp.maximum(entries, -limit), limit).astype(held_as)


def setup_inputs(seed: int = 0) -> dict:
    splits = jax.random.split(jax.random.key(seed), 13)
    conv_input = noise(splits[0], (CONV_TOKENS, D), 1.0, 6.0, ((0, 64), (1, 4)))
    conv_kernel = draw_conv_kernel(jax.random.fold_in(splits[12], 71), 0)
    norm_gain = jnp.clip(1.0 + 0.18 * jax.random.normal(splits[2], (D,), jnp.float32), 0.1, 1.9)
    norm_shift = noise(splits[3], (D,), 0.5, 3.0, ((0, 4),), jnp.float32)
    conv_proj = noise(splits[4], (D, D), D ** -0.5, 0.125, ((0, 4),))
    moe_input = noise(splits[5], (MOE_TOKENS, D), 1.0, 6.0, ((0, 256),))
    moe_gain = jnp.clip(1.0 + 0.18 * jax.random.normal(splits[6], (D,), jnp.float32), 0.1, 1.9)
    routes_keys = jax.random.split(jax.random.fold_in(splits[7], 1), MOE_TOKENS // (N_TP * TOK_DEV))
    routes_turns = jax.random.permutation(jax.random.fold_in(splits[7], 3), MOE_TOKENS // (N_TP * TOK_DEV))
    routes = jax.vmap(lambda own, number: assign_block(jax.random.fold_in(splits[7], 2), own, number, N_TP * TOK_DEV, EXPERTS, TOPK, CAPG, 2))(routes_keys, routes_turns).reshape((MOE_TOKENS, TOPK))
    route_weights = jnp.clip(0.2 + 0.8 * jax.random.uniform(splits[8], (MOE_TOKENS, TOPK), jnp.float32) ** shard_levels(splits[8], (MOE_TOKENS, TOPK), ((0, 64),), -0.2, 0.2), 0.2, 1.0)
    gate_proj = noise(splits[9], (EXPERTS, D, FE), D ** -0.5, 0.125, ((0, 64), (2, 4)))
    up_proj = noise(splits[10], (EXPERTS, D, FE), D ** -0.5, 0.125, ((0, 64), (2, 4)))
    down_proj = noise(splits[11], (EXPERTS, FE, D), FE ** -0.5, 0.125, ((0, 64), (1, 4)))
    return dict(conv_input=conv_input, conv_kernel=conv_kernel, norm_gain=norm_gain, norm_shift=norm_shift, conv_proj=conv_proj, moe_input=moe_input, moe_gain=moe_gain, routes=routes, route_weights=route_weights, gate_proj=gate_proj, up_proj=up_proj, down_proj=down_proj)


def conv_half(conv_input, conv_kernel, norm_gain, norm_shift, conv_proj):
    reach = CONV_WIDTH - 1
    padded = jnp.concatenate([jnp.zeros((reach, D), conv_input.dtype), conv_input], axis=0)
    taps = conv_kernel.astype(jnp.float32)
    mixed = jnp.zeros((CONV_TOKENS, D), jnp.float32)
    for offset in range(CONV_WIDTH):
        mixed = mixed + padded[offset:offset + CONV_TOKENS].astype(jnp.float32) * taps[offset]
    center = lax.optimization_barrier(jnp.sum(mixed, axis=1)) / D
    spread = jnp.maximum(lax.optimization_barrier(jnp.sum(mixed * mixed, axis=1)) / D - center * center, 0.0)
    scaled = (mixed - center[:, None]) * lax.rsqrt(spread[:, None] + 1e-05) * norm_gain + norm_shift
    activated = jax.nn.silu(scaled).astype(jnp.bfloat16)
    block = D // N_TP
    total = jnp.zeros((CONV_TOKENS, D), jnp.float32)
    for part in range(N_TP):
        piece = jnp.dot(activated[:, part * block:(part + 1) * block], conv_proj[part * block:(part + 1) * block], preferred_element_type=jnp.float32)
        total = total + lax.optimization_barrier(piece.astype(jnp.bfloat16)).astype(jnp.float32)
    return total.astype(jnp.bfloat16)

def moe_half(moe_input, moe_gain, routes, route_weights, gate_proj, up_proj, down_proj):
    moe_float = moe_input.astype(jnp.float32)
    normed = (moe_float * lax.rsqrt(lax.optimization_barrier(jnp.mean(moe_float * moe_float, axis=1, keepdims=True)) + 1e-06) * moe_gain).astype(jnp.bfloat16)
    block = FE // N_TP
    slots = N_EP * CAPG

    def one_expert(total, items):
        expert, gate_w, up_w, down_w = items
        hits = routes == expert
        weight = lax.optimization_barrier(jnp.sum(jnp.where(hits, route_weights, 0.0), axis=1))
        named = jnp.any(hits, axis=1)
        index = jnp.nonzero(named, size=slots, fill_value=0)[0].astype(jnp.int32)
        valid = jnp.arange(slots, dtype=jnp.int32) < jnp.sum(named.astype(jnp.int32))
        rows = normed[index]
        result = jnp.zeros((slots, D), jnp.float32)
        for part in range(N_TP):
            low = part * block
            gated = jax.nn.silu(jnp.dot(rows, gate_w[:, low:low + block], preferred_element_type=jnp.float32))
            hidden = (gated * jnp.dot(rows, up_w[:, low:low + block], preferred_element_type=jnp.float32)).astype(jnp.bfloat16)
            piece = jnp.dot(hidden, down_w[low:low + block], preferred_element_type=jnp.float32)
            result = result + lax.optimization_barrier(piece.astype(jnp.bfloat16)).astype(jnp.float32)
        scale = jnp.where(valid, weight[index], 0.0)
        return (total.at[index].add(result * scale[:, None]), None)
    experts = jnp.arange(EXPERTS, dtype=jnp.int32)
    total, _ = lax.scan(one_expert, jnp.zeros((MOE_TOKENS, D), jnp.float32), (experts, gate_proj, up_proj, down_proj))
    return total.astype(jnp.bfloat16)

def reference(conv_input, conv_kernel, norm_gain, norm_shift, conv_proj, moe_input, moe_gain, routes, route_weights, gate_proj, up_proj, down_proj):
    conv_out = conv_half(conv_input, conv_kernel, norm_gain, norm_shift, conv_proj)
    moe_out = moe_half(moe_input, moe_gain, routes, route_weights, gate_proj, up_proj, down_proj)
    return (conv_out, moe_out)
```

```python
import jax
import jax.numpy as jnp
from jax import lax
from jax.sharding import PartitionSpec as P

CHUNKS = 2


def shifted(value, axis, steps):
    count = lax.axis_size(axis)
    leading, last = (max(0, -steps), min(count, count - steps))
    return lax.ppermute(value, axis, [(source, source + steps) for source in range(leading, last)])


def dot(lhs, rhs):
    return jnp.dot(lhs, rhs, preferred_element_type=jnp.float32)


def in_three(value):
    high = lax.reduce_precision(value, 8, 7)
    rest = value - high
    middle = lax.reduce_precision(rest, 8, 7)
    low = rest - middle
    return [term.astype(jnp.bfloat16) for term in (high, middle, low)]


def tied(*values):
    return lax.optimization_barrier(values)


def local(
    conv_input,
    conv_kernel,
    norm_gain,
    norm_shift,
    conv_proj,
    moe_input,
    moe_gain,
    routes,
    route_weights,
    gate_proj,
    up_proj,
    down_proj,
):
    tp_count = lax.axis_size("tp")
    ep_count = lax.axis_size("ep")
    tp_index = lax.axis_index("tp")
    group_rows, top_count = routes.shape
    model_width = moe_input.shape[1]
    capacity = 2 * top_count * group_rows // ep_count
    share = capacity // tp_count
    per = share // CHUNKS

    moe_float = moe_input.astype(jnp.float32)
    normed = (
        moe_float
        * lax.rsqrt(jnp.mean(moe_float * moe_float, axis=1, keepdims=True) + 1e-06)
        * moe_gain
    ).astype(jnp.bfloat16)
    group = lax.all_gather(normed, "tp", axis=0, tiled=True)

    experts = jnp.arange(ep_count, dtype=jnp.int32)
    hits = routes.T[:, None, :] == experts[None, :, None]
    chosen = jnp.any(hits, axis=0)
    weight_of = jnp.sum(jnp.where(hits, route_weights.T[:, None, :], 0.0), axis=0)
    before = (
        lax.broadcasted_iota(jnp.int32, (group_rows, group_rows), 0)
        < lax.broadcasted_iota(jnp.int32, (group_rows, group_rows), 1)
    ).astype(jnp.bfloat16)
    rank = dot(chosen.astype(jnp.bfloat16), before).astype(jnp.int32)
    local_rank = jnp.where(chosen, rank - tp_index * share, -1)

    local_rows, local_width = conv_input.shape
    reach = conv_kernel.shape[0] - 1
    history = shifted(conv_input[local_rows - reach :], "ep", 1)
    padded = jnp.concatenate([history, conv_input], axis=0)
    taps = conv_kernel.astype(jnp.float32)
    mixed = jnp.zeros((local_rows, local_width), jnp.float32)
    for offset in range(reach + 1):
        mixed = mixed + padded[offset : offset + local_rows].astype(jnp.float32) * taps[offset]
    row_sums = (jnp.sum(mixed, axis=1), jnp.sum(mixed * mixed, axis=1))

    group, mixed, *row_sums = tied(group, mixed, *row_sums)

    landed, selected = [], []
    for chunk in range(CHUNKS):
        slots = chunk * per + jnp.arange(per, dtype=jnp.int32)
        select = local_rank[:, None, :] == slots[None, :, None]
        selected.append(select)
        rows = dot(
            select.astype(jnp.bfloat16).reshape(ep_count * per, group_rows), group
        ).astype(jnp.bfloat16)
        if chunk == 0:
            rows, *row_sums = tied(rows, *row_sums)
        landed.append(
            lax.all_to_all(
                rows.reshape(ep_count, per, model_width),
                "ep",
                split_axis=0,
                concat_axis=0,
                tiled=True,
            )
        )

    full_width = local_width * tp_count
    sums, squares = lax.psum(tuple(row_sums), "tp")
    center = sums / full_width
    spread = jnp.maximum(squares / full_width - center * center, 0.0)
    scaled = (mixed - center[:, None]) * lax.rsqrt(spread[:, None] + 1e-05) * norm_gain + norm_shift
    activated = jax.nn.silu(scaled).astype(jnp.bfloat16)
    projected = dot(activated, conv_proj).astype(jnp.bfloat16)
    landed[-1], projected = tied(landed[-1], projected)
    arrived = [lax.all_gather(part, "tp", axis=0, tiled=False) for part in landed]

    totals = []
    for chunk in range(CHUNKS):
        incoming = arrived[chunk].reshape(tp_count * ep_count * per, model_width)
        gated = jax.nn.silu(dot(incoming, gate_proj[0]))
        hidden = (gated * dot(incoming, up_proj[0])).astype(jnp.bfloat16)
        pieces = dot(hidden, down_proj[0]).astype(jnp.bfloat16)
        totals.append(lax.psum_scatter(pieces, "tp", scatter_dimension=0, tiled=True))

    projected, totals[-1] = tied(projected, totals[-1])
    conv_out = lax.psum_scatter(projected, "tp", scatter_dimension=0, tiled=True)

    combined = jnp.zeros((group_rows, model_width), jnp.float32)
    for chunk in range(CHUNKS):
        returned = lax.all_to_all(
            totals[chunk].reshape(ep_count, per, model_width),
            "ep",
            split_axis=0,
            concat_axis=0,
            tiled=True,
        ).reshape(ep_count * per, model_width)
        weights = jnp.where(selected[chunk], weight_of[:, None, :], 0.0)
        for term in in_three(weights.reshape(ep_count * per, group_rows)):
            combined = combined + lax.dot_general(
                term, returned, (((0,), (0,)), ((), ())), preferred_element_type=jnp.float32
            )
    combined, conv_out = tied(combined.astype(jnp.bfloat16), conv_out)
    moe_out = lax.psum_scatter(
        combined, "tp", scatter_dimension=0, tiled=True
    )
    return (conv_out, moe_out)


def solution(mesh):
    placed = (
        P("ep", "tp"),
        P(None, "tp"),
        P("tp"),
        P("tp"),
        P("tp", None),
        P(("ep", "tp"), None),
        P(),
        P("ep", None),
        P("ep", None),
        P("ep", None, "tp"),
        P("ep", None, "tp"),
        P("ep", "tp", None),
    )
    return jax.shard_map(
        local,
        mesh=mesh,
        in_specs=placed,
        out_specs=(P(("ep", "tp"), None), P(("ep", "tp"), None)),
        check_vma=False,
    )
```

```python
import jax
import jax.numpy as jnp
from jax import lax
from jax.sharding import PartitionSpec as P


def shifted(value, axis, steps):
    count = lax.axis_size(axis)
    leading, last = (max(0, -steps), min(count, count - steps))
    return lax.ppermute(value, axis, [(source, source + steps) for source in range(leading, last)])


def turned(value, steps):
    count = lax.axis_size("tp")
    return lax.ppermute(value, "tp", [(i, (i + steps) % count) for i in range(count)])


def dot(lhs, rhs):
    return jnp.dot(lhs, rhs, preferred_element_type=jnp.float32)


def in_three(value):
    high = lax.reduce_precision(value, 8, 7)
    rest = value - high
    middle = lax.reduce_precision(rest, 8, 7)
    low = rest - middle
    return [term.astype(jnp.bfloat16) for term in (high, middle, low)]


def tied(*values):
    return lax.optimization_barrier(values)


def rounded_sum(*values):
    return sum(value.astype(jnp.float32) for value in values).astype(jnp.bfloat16)


def summed_around(own, right, far, left):
    half = own.shape[0] // 2
    via_left = turned(far[:half], 1)
    via_right = turned(far[half:], -1)
    early_left = turned(right[half:], 1)
    early_right = turned(left[:half], -1)
    late_left = turned(rounded_sum(right[:half], via_left), 1)
    late_right = turned(rounded_sum(left[half:], via_right), -1)
    return jnp.concatenate(
        [
            rounded_sum(own[:half], late_left, early_right),
            rounded_sum(own[half:], early_left, late_right),
        ],
        axis=0,
    )


def local(
    conv_input,
    conv_kernel,
    norm_gain,
    norm_shift,
    conv_proj,
    moe_input,
    moe_gain,
    routes,
    route_weights,
    gate_proj,
    up_proj,
    down_proj,
):
    tp_count = lax.axis_size("tp")
    ep_count = lax.axis_size("ep")
    tp_index = lax.axis_index("tp")
    group_rows, top_count = routes.shape
    own_rows, model_width = moe_input.shape
    capacity = 2 * top_count * group_rows // ep_count
    share = capacity // tp_count
    slots = ep_count * share

    moe_float = moe_input.astype(jnp.float32)
    normed = (
        moe_float
        * lax.rsqrt(jnp.mean(moe_float * moe_float, axis=1, keepdims=True) + 1e-06)
        * moe_gain
    ).astype(jnp.bfloat16)
    from_left = turned(normed, 1)
    from_right = turned(normed, -1)

    experts = jnp.arange(ep_count, dtype=jnp.int32)
    hits = routes.T[:, None, :] == experts[None, :, None]
    chosen = jnp.any(hits, axis=0)
    weight_of = jnp.sum(jnp.where(hits, route_weights.T[:, None, :], 0.0), axis=0)
    before = (
        lax.broadcasted_iota(jnp.int32, (group_rows, group_rows), 0)
        < lax.broadcasted_iota(jnp.int32, (group_rows, group_rows), 1)
    ).astype(jnp.bfloat16)
    rank = dot(chosen.astype(jnp.bfloat16), before).astype(jnp.int32)
    local_rank = jnp.where(chosen, rank - tp_index * share, -1)

    def from_here(table):
        return lax.dynamic_slice_in_dim(
            jnp.concatenate([table, table], axis=1), tp_index * own_rows, group_rows, axis=1
        )

    select = (
        from_here(local_rank)[:, None, :] == jnp.arange(share, dtype=jnp.int32)[None, :, None]
    )
    weights = jnp.where(select, from_here(weight_of)[:, None, :], 0.0)
    select = select.astype(jnp.bfloat16).reshape(slots, group_rows)
    weights = weights.reshape(slots, group_rows)

    local_rows, local_width = conv_input.shape
    reach = conv_kernel.shape[0] - 1
    history = shifted(conv_input[local_rows - reach :], "ep", 1)
    taps = conv_kernel.astype(jnp.float32)

    def convolved(window):
        rows = window.shape[0] - reach
        mixed = jnp.zeros((rows, local_width), jnp.float32)
        for offset in range(reach + 1):
            mixed = mixed + window[offset : offset + rows].astype(jnp.float32) * taps[offset]
        return mixed, jnp.sum(mixed, axis=1), jnp.sum(mixed * mixed, axis=1)

    middle = local_rows // 2
    second = convolved(conv_input[middle - reach :])
    from_left, from_right, *second = tied(from_left, from_right, *second)
    half = own_rows // 2
    far = jnp.concatenate([turned(from_left[:half], 1), turned(from_right[half:], -1)], axis=0)
    head, _ = tied(conv_input[:middle], second[1])
    first = convolved(jnp.concatenate([history, head], axis=0))
    far, *first = tied(far, *first)

    group = jnp.concatenate([normed, from_right, far, from_left], axis=0)
    rows = dot(select, group).astype(jnp.bfloat16)
    row_sums = [jnp.concatenate(pair) for pair in zip(first[1:], second[1:])]
    rows, *row_sums = tied(rows, *row_sums)
    landed = lax.all_to_all(
        rows.reshape(ep_count, share, model_width), "ep", split_axis=0, concat_axis=0, tiled=True
    )

    full_width = local_width * tp_count
    sums, squares = lax.psum(tuple(row_sums), "tp")
    center = sums / full_width
    spread = jnp.maximum(squares / full_width - center * center, 0.0)
    mixed = jnp.concatenate([first[0], second[0]], axis=0)
    scaled = (mixed - center[:, None]) * lax.rsqrt(spread[:, None] + 1e-05) * norm_gain + norm_shift
    activated = jax.nn.silu(scaled).astype(jnp.bfloat16)
    block = local_rows // tp_count
    projected = []
    for step in range(tp_count):
        start = lax.rem(tp_index + step, tp_count) * block
        part = lax.dynamic_slice_in_dim(activated, start, block, axis=0)
        projected.append(dot(part, conv_proj).astype(jnp.bfloat16))
    landed, *projected = tied(landed, *projected)

    def expert(incoming):
        gated = jax.nn.silu(dot(incoming, gate_proj[0]))
        hidden = (gated * dot(incoming, up_proj[0])).astype(jnp.bfloat16)
        return dot(hidden, down_proj[0]).astype(jnp.bfloat16)

    landed = landed.reshape(slots, model_width)
    at_left = turned(landed, 1)
    at_right = turned(landed, -1)
    piece_own = expert(landed)
    half = slots // 2
    at_left, at_right, piece_own = tied(at_left, at_right, piece_own)
    at_far = jnp.concatenate([turned(at_left[:half], 1), turned(at_right[half:], -1)], axis=0)
    piece_right = expert(at_right)
    piece_left = expert(at_left)
    piece_far = expert(at_far)
    totals = summed_around(piece_own, piece_right, piece_far, piece_left)

    totals, *projected = tied(totals, *projected)
    returned = lax.all_to_all(
        totals.reshape(ep_count, share, model_width), "ep", split_axis=0, concat_axis=0, tiled=True
    ).reshape(slots, model_width)
    conv_out = summed_around(*projected)
    returned, conv_out = tied(returned, conv_out)

    combined = jnp.zeros((group_rows, model_width), jnp.float32)
    for term in in_three(weights):
        combined = combined + lax.dot_general(
            term, returned, (((0,), (0,)), ((), ())), preferred_element_type=jnp.float32
        )
    combined = combined.astype(jnp.bfloat16)
    moe_out = summed_around(
        *(combined[step * own_rows : (step + 1) * own_rows] for step in range(tp_count))
    )
    return (conv_out, moe_out)


def solution(mesh):
    placed = (
        P("ep", "tp"),
        P(None, "tp"),
        P("tp"),
        P("tp"),
        P("tp", None),
        P(("ep", "tp"), None),
        P(),
        P("ep", None),
        P("ep", None),
        P("ep", None, "tp"),
        P("ep", None, "tp"),
        P("ep", "tp", None),
    )
    return jax.shard_map(
        local,
        mesh=mesh,
        in_specs=placed,
        out_specs=(P(("ep", "tp"), None), P(("ep", "tp"), None)),
        check_vma=False,
    )
```

```python
import jax
import jax.numpy as jnp
from jax import lax
from jax.experimental import pallas as pl
from jax.experimental.pallas import tpu as pltpu
from jax.sharding import PartitionSpec as P


def shifted(value, axis, steps):
    count = lax.axis_size(axis)
    leading, last = (max(0, -steps), min(count, count - steps))
    return lax.ppermute(value, axis, [(source, source + steps) for source in range(leading, last)])


def turned(value, steps):
    count = lax.axis_size("tp")
    return lax.ppermute(value, "tp", [(i, (i + steps) % count) for i in range(count)])


def dot(lhs, rhs):
    return jnp.dot(lhs, rhs, preferred_element_type=jnp.float32)


def in_three(value):
    high = lax.reduce_precision(value, 8, 7)
    rest = value - high
    middle = lax.reduce_precision(rest, 8, 7)
    low = rest - middle
    return [term.astype(jnp.bfloat16) for term in (high, middle, low)]


def tied(*values):
    return lax.optimization_barrier(values)


def rounded_sum(*values):
    return sum(value.astype(jnp.float32) for value in values).astype(jnp.bfloat16)


def ring_sum(own, right, far, left):
    early_left = turned(right[1], 1)
    early_right = turned(left[0], -1)
    via_left = turned(far[0], 1)
    via_right = turned(far[1], -1)
    late_left = turned(rounded_sum(right[0], via_left), 1)
    late_right = turned(rounded_sum(left[1], via_right), -1)
    return (
        rounded_sum(own[0], late_left, early_right),
        rounded_sum(own[1], early_left, late_right),
    )


def expert_body(top_ref, low_ref, gate_ref, up_ref, down_ref, top_out, low_out, rows, total):
    step = pl.program_id(0)
    half = top_ref.shape[0]

    @pl.when(step == 0)
    def _():
        rows[:half] = top_ref[...]
        rows[half:] = low_ref[...]

    gated = dot(rows[...], gate_ref[0])
    raised = dot(rows[...], up_ref[0])
    hidden = (gated / (1.0 + jnp.exp(-gated)) * raised).astype(jnp.bfloat16)
    added = dot(hidden, down_ref[0])

    @pl.when(step == 0)
    def _():
        total[...] = added

    @pl.when(step == pl.num_programs(0) - 1)
    def _():
        top_out[...] = (total[:half] + added[:half]).astype(jnp.bfloat16)
        low_out[...] = (total[half:] + added[half:]).astype(jnp.bfloat16)


def expert(top, low, gate_proj, up_proj, down_proj):
    half, width = top.shape
    hidden = gate_proj.shape[2]
    steps = 2
    tile = hidden // steps
    block = pl.BlockSpec((half, width), lambda i: (0, 0))
    shape = jax.ShapeDtypeStruct((half, width), jnp.bfloat16)
    return pl.pallas_call(
        expert_body,
        grid=(steps,),
        in_specs=[
            block,
            block,
            pl.BlockSpec((1, width, tile), lambda i: (0, 0, i)),
            pl.BlockSpec((1, width, tile), lambda i: (0, 0, i)),
            pl.BlockSpec((1, tile, width), lambda i: (0, i, 0)),
        ],
        out_specs=[block, block],
        out_shape=[shape, shape],
        scratch_shapes=[
            pltpu.VMEM((2 * half, width), jnp.bfloat16),
            pltpu.VMEM((2 * half, width), jnp.float32),
        ],
        compiler_params=pltpu.CompilerParams(
            dimension_semantics=("arbitrary",), vmem_limit_bytes=32 * 1024 * 1024
        ),
        cost_estimate=pl.CostEstimate(
            flops=12 * half * width * hidden,
            bytes_accessed=6 * width * hidden + 8 * half * width,
            transcendentals=2 * half * hidden,
        ),
        name="expert",
    )(top, low, gate_proj, up_proj, down_proj)


def taps_body(rows_ref, history_ref, taps_ref, mixed_ref, sums_ref, squares_ref, window):
    count, width = rows_ref.shape
    reach = taps_ref.shape[1] - 1
    lead = history_ref.shape[0]
    lanes = window.shape[2]
    tiles = width // lanes
    for tile in range(tiles):
        columns = slice(tile * lanes, (tile + 1) * lanes)
        window[tile, :lead] = history_ref[:, columns].astype(jnp.float32)
        window[tile, lead:] = rows_ref[:, columns].astype(jnp.float32)
    block = 128
    ones = jnp.ones((8, lanes), jnp.float32)

    def across_lanes(value):
        return lax.dot_general(
            ones,
            value,
            (((1,), (1,)), ((), ())),
            precision=lax.Precision.HIGHEST,
            preferred_element_type=jnp.float32,
        )[0:1]

    @pl.loop(0, count // block)
    def _(step):
        base = step * block

        def one(tile, carry):
            total = jnp.zeros((block, lanes), jnp.float32)
            for offset in range(reach + 1):
                part = window[tile, pl.ds(base + (lead - reach + offset), block), :]
                total = total + part * taps_ref[tile, offset : offset + 1, :]
            at = pl.multiple_of(base, block)
            mixed_ref[tile, pl.ds(at, block), :] = total
            return carry

        lax.fori_loop(0, tiles, one, 0)
        at = pl.multiple_of(base, block)
        parts = [mixed_ref[tile, pl.ds(at, block), :] for tile in range(tiles)]
        sums_ref[pl.ds(step, 1), :] = across_lanes(sum(parts))
        squares_ref[pl.ds(step, 1), :] = across_lanes(sum(part * part for part in parts))


def convolved(rows, history, taps):
    count, width = rows.shape
    lanes = 128
    tiles = width // lanes
    taps = jnp.moveaxis(taps.astype(jnp.float32).reshape(-1, tiles, lanes), 1, 0)
    stats = jax.ShapeDtypeStruct((count // 128, 128), jnp.float32)
    return pl.pallas_call(
        taps_body,
        out_shape=[jax.ShapeDtypeStruct((tiles, count, lanes), jnp.float32), stats, stats],
        scratch_shapes=[pltpu.VMEM((tiles, count + history.shape[0], lanes), jnp.float32)],
        compiler_params=pltpu.CompilerParams(vmem_limit_bytes=32 * 1024 * 1024),
        cost_estimate=pl.CostEstimate(
            flops=400 * taps.shape[1] * count * width,
            bytes_accessed=6 * count * width,
            transcendentals=0,
        ),
        name="taps",
    )(rows, history, taps)


def local(
    conv_input,
    conv_kernel,
    norm_gain,
    norm_shift,
    conv_proj,
    moe_input,
    moe_gain,
    routes,
    route_weights,
    gate_proj,
    up_proj,
    down_proj,
):
    tp_count = lax.axis_size("tp")
    ep_count = lax.axis_size("ep")
    tp_index = lax.axis_index("tp")
    group_rows, top_count = routes.shape
    own_rows, model_width = moe_input.shape
    capacity = 2 * top_count * group_rows // ep_count
    share = capacity // tp_count
    slots = ep_count * share

    moe_float = moe_input.astype(jnp.float32)
    normed = (
        moe_float
        * lax.rsqrt(jnp.mean(moe_float * moe_float, axis=1, keepdims=True) + 1e-06)
        * moe_gain
    ).astype(jnp.bfloat16)
    group = lax.all_to_all(
        jnp.broadcast_to(normed[None], (tp_count, own_rows, model_width)), "tp", 0, 0, tiled=True
    ).reshape(group_rows, model_width)

    experts = jnp.arange(ep_count, dtype=jnp.int32)
    hits = routes.T[:, None, :] == experts[None, :, None]
    chosen = jnp.any(hits, axis=0)
    weight_of = jnp.sum(jnp.where(hits, route_weights.T[:, None, :], 0.0), axis=0)
    before = (
        lax.broadcasted_iota(jnp.int32, (group_rows, group_rows), 0)
        < lax.broadcasted_iota(jnp.int32, (group_rows, group_rows), 1)
    ).astype(jnp.bfloat16)
    rank = dot(chosen.astype(jnp.bfloat16), before).astype(jnp.int32)
    local_rank = jnp.where(chosen, rank - tp_index * share, -1)
    select = local_rank[:, None, :] == jnp.arange(share, dtype=jnp.int32)[None, :, None]
    weights = jnp.where(select, weight_of[:, None, :], 0.0).reshape(slots, group_rows)
    select = select.astype(jnp.bfloat16).reshape(slots, group_rows)

    rows = dot(select, group).astype(jnp.bfloat16)
    rows, conv_input = tied(rows, conv_input)
    landed = lax.all_to_all(
        rows.reshape(ep_count, share, model_width), "ep", split_axis=0, concat_axis=0, tiled=True
    )

    local_rows, local_width = conv_input.shape
    history = shifted(conv_input[local_rows - 32 :], "ep", 1)
    mixed, *stats = convolved(conv_input, history, conv_kernel)
    full_width = local_width * tp_count
    sums, squares = lax.psum(tuple(stats), "tp")
    landed, mixed, sums, squares = tied(landed, mixed, sums, squares)

    near = ep_count // 2
    own = [part.reshape(near * share, model_width) for part in (landed[:near], landed[near:])]
    left_top, right_low = turned(own[0], 1), turned(own[1], -1)
    left_low, right_top = turned(own[1], 1), turned(own[0], -1)
    matrices = (gate_proj, up_proj, down_proj)
    own = expert(*own, *matrices)
    left_top, right_low, *own = tied(left_top, right_low, *own)
    far_top, far_low = turned(left_top, 1), turned(right_low, -1)
    left_top, right_low = expert(left_top, right_low, *matrices)
    left_top, right_low, right_top, left_low = tied(left_top, right_low, right_top, left_low)
    right_top, left_low = expert(right_top, left_low, *matrices)
    far_top, far_low, right_top, left_low = tied(far_top, far_low, right_top, left_low)
    far = expert(far_top, far_low, *matrices)

    mixed, sums, squares, *far = tied(mixed, sums, squares, *far)
    center = sums / full_width
    spread = jnp.maximum(squares / full_width - center * center, 0.0)
    factor = lax.rsqrt(spread + 1e-05)
    mixed = jnp.concatenate(list(mixed), axis=1)
    scaled = (mixed - center.reshape(-1, 1)) * factor.reshape(-1, 1) * norm_gain + norm_shift
    activated = jax.nn.silu(scaled).astype(jnp.bfloat16)
    half = local_rows // (2 * tp_count)
    projected = []
    for step in range(tp_count):
        start = lax.rem(tp_index + step, tp_count) * (2 * half)
        part = lax.dynamic_slice_in_dim(activated, start, 2 * half, axis=0)
        part = dot(part, conv_proj).astype(jnp.bfloat16)
        projected.append((part[:half], part[half:]))

    totals = ring_sum(own, (right_top, right_low), far, (left_top, left_low))
    flat = tied(*totals, *(part for pair in projected for part in pair))
    totals, projected = flat[:2], [flat[2 + 2 * i : 4 + 2 * i] for i in range(tp_count)]

    returned = lax.all_to_all(
        jnp.concatenate([part.reshape(near, share, model_width) for part in totals], axis=0),
        "ep",
        split_axis=0,
        concat_axis=0,
        tiled=True,
    ).reshape(slots, model_width)
    conv_out = jnp.concatenate(ring_sum(*projected), axis=0)
    returned, conv_out = tied(returned, conv_out)

    combined = jnp.zeros((group_rows, model_width), jnp.float32)
    for term in in_three(weights):
        combined = combined + lax.dot_general(
            term, returned, (((0,), (0,)), ((), ())), preferred_element_type=jnp.float32
        )
    parts = lax.all_to_all(
        combined.astype(jnp.bfloat16).reshape(tp_count, own_rows, model_width), "tp", 0, 0, tiled=True
    )
    moe_out = jnp.sum(parts.astype(jnp.float32), axis=0).astype(jnp.bfloat16)
    return (conv_out, moe_out)


def solution(mesh):
    placed = (
        P("ep", "tp"),
        P(None, "tp"),
        P("tp"),
        P("tp"),
        P("tp", None),
        P(("ep", "tp"), None),
        P(),
        P("ep", None),
        P("ep", None),
        P("ep", None, "tp"),
        P("ep", None, "tp"),
        P("ep", "tp", None),
    )
    return jax.shard_map(
        local,
        mesh=mesh,
        in_specs=placed,
        out_specs=(P(("ep", "tp"), None), P(("ep", "tp"), None)),
        check_vma=False,
    )
```

```python
import jax
import jax.numpy as jnp
from jax import lax
from jax.experimental import pallas as pl
from jax.experimental.pallas import tpu as pltpu
from jax.sharding import PartitionSpec as P


def shifted(value, axis, steps):
    count = lax.axis_size(axis)
    leading, last = (max(0, -steps), min(count, count - steps))
    return lax.ppermute(value, axis, [(source, source + steps) for source in range(leading, last)])


def turned(value, steps):
    count = lax.axis_size("tp")
    return lax.ppermute(value, "tp", [(i, (i + steps) % count) for i in range(count)])


def dot(lhs, rhs):
    return jnp.dot(lhs, rhs, preferred_element_type=jnp.float32)


def in_three(value):
    high = lax.reduce_precision(value, 8, 7)
    rest = value - high
    middle = lax.reduce_precision(rest, 8, 7)
    low = rest - middle
    return [term.astype(jnp.bfloat16) for term in (high, middle, low)]


def tied(*values):
    return lax.optimization_barrier(values)


def rounded_sum(*values):
    return sum(value.astype(jnp.float32) for value in values).astype(jnp.bfloat16)


def expert_body(top_ref, low_ref, gate_ref, up_ref, down_ref, top_out, low_out, rows, total):
    step = pl.program_id(0)
    half = top_ref.shape[0]

    @pl.when(step == 0)
    def _():
        rows[:half] = top_ref[...]
        rows[half:] = low_ref[...]

    gated = dot(rows[...], gate_ref[0])
    raised = dot(rows[...], up_ref[0])
    hidden = (gated / (1.0 + jnp.exp(-gated)) * raised).astype(jnp.bfloat16)
    added = dot(hidden, down_ref[0])

    @pl.when(step == 0)
    def _():
        total[...] = added

    @pl.when(step == pl.num_programs(0) - 1)
    def _():
        top_out[...] = (total[:half] + added[:half]).astype(jnp.bfloat16)
        low_out[...] = (total[half:] + added[half:]).astype(jnp.bfloat16)


def expert(top, low, gate_proj, up_proj, down_proj):
    half, width = top.shape
    hidden = gate_proj.shape[2]
    steps = 2
    tile = hidden // steps
    block = pl.BlockSpec((half, width), lambda i: (0, 0))
    shape = jax.ShapeDtypeStruct((half, width), jnp.bfloat16)
    return pl.pallas_call(
        expert_body,
        grid=(steps,),
        in_specs=[
            block,
            block,
            pl.BlockSpec((1, width, tile), lambda i: (0, 0, i)),
            pl.BlockSpec((1, width, tile), lambda i: (0, 0, i)),
            pl.BlockSpec((1, tile, width), lambda i: (0, i, 0)),
        ],
        out_specs=[block, block],
        out_shape=[shape, shape],
        scratch_shapes=[
            pltpu.VMEM((2 * half, width), jnp.bfloat16),
            pltpu.VMEM((2 * half, width), jnp.float32),
        ],
        compiler_params=pltpu.CompilerParams(
            dimension_semantics=("arbitrary",), vmem_limit_bytes=32 * 1024 * 1024
        ),
        cost_estimate=pl.CostEstimate(
            flops=12 * half * width * hidden,
            bytes_accessed=6 * width * hidden + 8 * half * width,
            transcendentals=2 * half * hidden,
        ),
        name="expert",
    )(top, low, gate_proj, up_proj, down_proj)


def taps_body(rows_ref, history_ref, taps_ref, mixed_ref, sums_ref, squares_ref, window, taps):
    count, width = rows_ref.shape
    reach = taps_ref.shape[0] - 1
    lead = history_ref.shape[0]
    lanes = window.shape[2]
    tiles = width // lanes
    for tile in range(tiles):
        columns = slice(tile * lanes, (tile + 1) * lanes)
        window[tile, :lead] = history_ref[:, columns].astype(jnp.float32)
        window[tile, lead:] = rows_ref[:, columns].astype(jnp.float32)
        taps[tile, : reach + 1] = taps_ref[:, columns].astype(jnp.float32)
    block = 128
    ones = jnp.ones((8, lanes), jnp.float32)

    def across_lanes(value):
        return lax.dot_general(
            ones,
            value,
            (((1,), (1,)), ((), ())),
            precision=lax.Precision.HIGHEST,
            preferred_element_type=jnp.float32,
        )[0:1]

    @pl.loop(0, count // block)
    def _(step):
        base = step * block

        def one(tile, carry):
            total = jnp.zeros((block, lanes), jnp.float32)
            for offset in range(reach + 1):
                part = window[tile, pl.ds(base + (lead - reach + offset), block), :]
                total = total + part * taps[tile, offset : offset + 1, :]
            at = pl.multiple_of(base, block)
            mixed_ref[tile, pl.ds(at, block), :] = total
            return carry

        lax.fori_loop(0, tiles, one, 0)
        at = pl.multiple_of(base, block)
        parts = [mixed_ref[tile, pl.ds(at, block), :] for tile in range(tiles)]
        sums_ref[pl.ds(step, 1), :] = across_lanes(sum(parts))
        squares_ref[pl.ds(step, 1), :] = across_lanes(sum(part * part for part in parts))


def convolved(rows, history, taps):
    count, width = rows.shape
    lanes = 128
    tiles = width // lanes
    stats = jax.ShapeDtypeStruct((count // 128, 128), jnp.float32)
    return pl.pallas_call(
        taps_body,
        out_shape=[jax.ShapeDtypeStruct((tiles, count, lanes), jnp.float32), stats, stats],
        scratch_shapes=[
            pltpu.VMEM((tiles, count + history.shape[0], lanes), jnp.float32),
            pltpu.VMEM((tiles, 32, lanes), jnp.float32),
        ],
        compiler_params=pltpu.CompilerParams(vmem_limit_bytes=32 * 1024 * 1024),
        cost_estimate=pl.CostEstimate(
            flops=400 * taps.shape[0] * count * width,
            bytes_accessed=6 * count * width,
            transcendentals=0,
        ),
        name="taps",
    )(rows, history, taps)


def pick_body(select_ref, group_ref, out_ref):
    width = group_ref.shape[1]
    wide = 512
    for start in range(0, width, wide):
        columns = slice(start, start + wide)
        picked = dot(select_ref[...], group_ref[:, columns]).astype(jnp.bfloat16)
        out_ref[:, :, columns] = picked.reshape(out_ref.shape[0], out_ref.shape[1], wide)


def picked(select, group, share):
    slots, width = select.shape[0], group.shape[1]
    return pl.pallas_call(
        pick_body,
        out_shape=jax.ShapeDtypeStruct((slots // share, share, width), jnp.bfloat16),
        cost_estimate=pl.CostEstimate(
            flops=2 * slots * select.shape[1] * width,
            bytes_accessed=4 * slots * width,
            transcendentals=0,
        ),
        name="pick",
    )(select, group)


def halves_body(whole_ref, top_ref, low_ref):
    near = whole_ref.shape[0] // 2
    top_ref[...] = whole_ref[:near].reshape(top_ref.shape)
    low_ref[...] = whole_ref[near:].reshape(low_ref.shape)


def halves(whole):
    peers, share, width = whole.shape
    shape = jax.ShapeDtypeStruct((peers * share // 2, width), jnp.bfloat16)
    return pl.pallas_call(halves_body, out_shape=[shape, shape], name="halves")(whole)


def close_body(*refs):
    out_ref = refs[-1]
    near = out_ref.shape[0] // 2
    for index in range(2):
        terms = [ref[...].astype(jnp.float32) for ref in refs[3 * index : 3 * index + 3]]
        whole = (terms[0] + terms[1] + terms[2]).astype(jnp.bfloat16)
        out_ref[near * index : near * (index + 1)] = whole.reshape(near, *out_ref.shape[1:])


def closed(top, low, peers):
    rows, width = top[0].shape
    return pl.pallas_call(
        close_body,
        out_shape=jax.ShapeDtypeStruct((peers, 2 * rows // peers, width), jnp.bfloat16),
        name="close",
    )(*top, *low)


def mix_body(returned_ref, *refs):
    out_ref = refs[-1]
    slots = returned_ref.shape[0] * returned_ref.shape[1]
    width = returned_ref.shape[2]
    wide = 512
    for start in range(0, width, wide):
        columns = slice(start, start + wide)
        rows = returned_ref[:, :, columns].reshape(slots, wide)
        total = sum(
            lax.dot_general(
                ref[...], rows, (((0,), (0,)), ((), ())), preferred_element_type=jnp.float32
            )
            for ref in refs[:3]
        )
        out_ref[:, columns] = total.astype(jnp.bfloat16)


def mixed_in(returned, terms):
    width = returned.shape[2]
    return pl.pallas_call(
        mix_body,
        out_shape=jax.ShapeDtypeStruct((terms[0].shape[1], width), jnp.bfloat16),
        name="mix",
    )(returned, *terms)


def local(
    conv_input,
    conv_kernel,
    norm_gain,
    norm_shift,
    conv_proj,
    moe_input,
    moe_gain,
    routes,
    route_weights,
    gate_proj,
    up_proj,
    down_proj,
):
    tp_count = lax.axis_size("tp")
    ep_count = lax.axis_size("ep")
    tp_index = lax.axis_index("tp")
    group_rows, top_count = routes.shape
    own_rows, model_width = moe_input.shape
    capacity = 2 * top_count * group_rows // ep_count
    share = capacity // tp_count
    slots = ep_count * share

    moe_float = moe_input.astype(jnp.float32)
    normed = (
        moe_float
        * lax.rsqrt(jnp.mean(moe_float * moe_float, axis=1, keepdims=True) + 1e-06)
        * moe_gain
    ).astype(jnp.bfloat16)
    group = lax.all_to_all(
        jnp.broadcast_to(normed[None], (tp_count, own_rows, model_width)), "tp", 0, 0, tiled=True
    ).reshape(group_rows, model_width)

    experts = jnp.arange(ep_count, dtype=jnp.int32)
    hits = routes.T[:, None, :] == experts[None, :, None]
    chosen = jnp.any(hits, axis=0)
    before = (
        lax.broadcasted_iota(jnp.int32, (group_rows, group_rows), 0)
        < lax.broadcasted_iota(jnp.int32, (group_rows, group_rows), 1)
    ).astype(jnp.bfloat16)
    rank = dot(chosen.astype(jnp.bfloat16), before).astype(jnp.int32)
    local_rank = jnp.where(chosen, rank - tp_index * share, -1)
    select = local_rank[:, None, :] == jnp.arange(share, dtype=jnp.int32)[None, :, None]
    select = select.astype(jnp.bfloat16).reshape(slots, group_rows)

    local_rows, local_width = conv_input.shape
    history = shifted(conv_input[local_rows - 32 :], "ep", 1)
    mixed, *stats = convolved(conv_input, history, conv_kernel)
    group, select, mixed, *stats = tied(group, select, mixed, *stats)

    rows = picked(select, group, share)
    rows, routes, route_weights, *stats = tied(rows, routes, route_weights, *stats)
    landed = lax.all_to_all(rows, "ep", split_axis=0, concat_axis=0, tiled=True)

    hits = routes.T[:, None, :] == experts[None, :, None]
    weight_of = jnp.sum(jnp.where(hits, route_weights.T[:, None, :], 0.0), axis=0)
    weights = jnp.repeat(weight_of, share, axis=0) * select.astype(jnp.float32)
    terms = in_three(weights)

    full_width = local_width * tp_count
    sums, squares = lax.psum(tuple(stats), "tp")
    center = sums / full_width
    spread = jnp.maximum(squares / full_width - center * center, 0.0)
    factor = lax.rsqrt(spread + 1e-05)
    mixed = jnp.concatenate(list(mixed), axis=1)
    scaled = (mixed - center.reshape(-1, 1)) * factor.reshape(-1, 1) * norm_gain + norm_shift
    activated = jax.nn.silu(scaled).astype(jnp.bfloat16)
    half = local_rows // (2 * tp_count)

    def projected(step):
        start = lax.rem(tp_index + step, tp_count) * (2 * half)
        pair = []
        for offset in (0, half):
            part = lax.dynamic_slice_in_dim(activated, start + offset, half, axis=0)
            pair.append(dot(part, conv_proj).astype(jnp.bfloat16))
        return pair

    conv_far = projected(2)
    conv_right = projected(1)
    conv_left = projected(3)
    conv_own = projected(0)
    via_left = turned(conv_far[0], 1)
    via_right = turned(conv_far[1], -1)
    conv_right[0] = rounded_sum(conv_right[0], via_left)
    conv_left[1] = rounded_sum(conv_left[1], via_right)
    landed, *terms = tied(landed, *terms)
    landed, *rest = tied(landed, *conv_right, *conv_left, *conv_own)
    conv_right, conv_left, conv_own = rest[:2], rest[2:4], rest[4:]

    own = halves(landed)
    left_top, right_low = turned(own[0], 1), turned(own[1], -1)
    left_low, right_top = turned(own[1], 1), turned(own[0], -1)
    matrices = (gate_proj, up_proj, down_proj)
    own = expert(*own, *matrices)
    left_top, right_low, *own = tied(left_top, right_low, *own)
    far_top, far_low = turned(left_top, 1), turned(right_low, -1)
    left_top, right_low = expert(left_top, right_low, *matrices)
    left_top, right_low, right_top, left_low = tied(left_top, right_low, right_top, left_low)
    early_left, early_right = turned(right_low, 1), turned(left_top, -1)
    right_top, left_low = expert(right_top, left_low, *matrices)
    far_top, far_low, right_top, left_low = tied(far_top, far_low, right_top, left_low)
    far_top, far_low = expert(far_top, far_low, *matrices)

    right_top = rounded_sum(right_top, turned(far_top, 1))
    left_low = rounded_sum(left_low, turned(far_low, -1))
    flat = tied(right_top, left_low, *conv_right, *conv_left)
    right_top, left_low, conv_right, conv_left = flat[0], flat[1], flat[2:4], flat[4:6]
    late_left, late_right = turned(right_top, 1), turned(left_low, -1)
    conv_top = [turned(conv_right[0], 1), turned(conv_left[0], -1)]
    conv_low = [turned(conv_right[1], 1), turned(conv_left[1], -1)]
    totals = closed((own[0], late_left, early_right), (own[1], early_left, late_right), ep_count)

    returned = lax.all_to_all(totals, "ep", split_axis=0, concat_axis=0, tiled=True)
    combined = mixed_in(returned, terms)
    conv_out = jnp.concatenate(
        [rounded_sum(conv_own[0], *conv_top), rounded_sum(conv_own[1], *conv_low)], axis=0
    )
    parts = lax.all_to_all(
        combined.reshape(tp_count, own_rows, model_width), "tp", 0, 0, tiled=True
    )
    parts, conv_out = tied(parts, conv_out)
    moe_out = jnp.sum(parts.astype(jnp.float32), axis=0).astype(jnp.bfloat16)
    return (conv_out, moe_out)


def solution(mesh):
    placed = (
        P("ep", "tp"),
        P(None, "tp"),
        P("tp"),
        P("tp"),
        P("tp", None),
        P(("ep", "tp"), None),
        P(),
        P("ep", None),
        P("ep", None),
        P("ep", None, "tp"),
        P("ep", None, "tp"),
        P("ep", "tp", None),
    )
    return jax.shard_map(
        local,
        mesh=mesh,
        in_specs=placed,
        out_specs=(P(("ep", "tp"), None), P(("ep", "tp"), None)),
        check_vma=False,
    )
```

```python
import jax
import jax.numpy as jnp
from jax import lax
from jax.experimental import pallas as pl
from jax.experimental.pallas import tpu as pltpu
from jax.sharding import PartitionSpec as P


def shifted(value, axis, steps):
    count = lax.axis_size(axis)
    leading, last = (max(0, -steps), min(count, count - steps))
    return lax.ppermute(value, axis, [(source, source + steps) for source in range(leading, last)])


def turned(value, steps):
    count = lax.axis_size("tp")
    return lax.ppermute(value, "tp", [(i, (i + steps) % count) for i in range(count)])


def dot(lhs, rhs):
    return jnp.dot(lhs, rhs, preferred_element_type=jnp.float32)


def in_three(value):
    high = lax.reduce_precision(value, 8, 7)
    rest = value - high
    middle = lax.reduce_precision(rest, 8, 7)
    low = rest - middle
    return [term.astype(jnp.bfloat16) for term in (high, middle, low)]


def tied(*values):
    return lax.optimization_barrier(values)


def rounded_sum(*values):
    return sum(value.astype(jnp.float32) for value in values).astype(jnp.bfloat16)


def expert_body(top_ref, low_ref, gate_ref, up_ref, down_ref, top_out, low_out, rows, total):
    step = pl.program_id(0)
    half = top_ref.shape[0]

    @pl.when(step == 0)
    def _():
        rows[:half] = top_ref[...]
        rows[half:] = low_ref[...]

    gated = dot(rows[...], gate_ref[0])
    raised = dot(rows[...], up_ref[0])
    hidden = (gated / (1.0 + jnp.exp(-gated)) * raised).astype(jnp.bfloat16)
    added = dot(hidden, down_ref[0])

    @pl.when(step == 0)
    def _():
        total[...] = added

    @pl.when(step == pl.num_programs(0) - 1)
    def _():
        top_out[...] = (total[:half] + added[:half]).astype(jnp.bfloat16)
        low_out[...] = (total[half:] + added[half:]).astype(jnp.bfloat16)


def expert(top, low, gate_proj, up_proj, down_proj):
    half, width = top.shape
    hidden = gate_proj.shape[2]
    steps = 2
    tile = hidden // steps
    block = pl.BlockSpec((half, width), lambda i: (0, 0))
    shape = jax.ShapeDtypeStruct((half, width), jnp.bfloat16)
    return pl.pallas_call(
        expert_body,
        grid=(steps,),
        in_specs=[
            block,
            block,
            pl.BlockSpec((1, width, tile), lambda i: (0, 0, i)),
            pl.BlockSpec((1, width, tile), lambda i: (0, 0, i)),
            pl.BlockSpec((1, tile, width), lambda i: (0, i, 0)),
        ],
        out_specs=[block, block],
        out_shape=[shape, shape],
        scratch_shapes=[
            pltpu.VMEM((2 * half, width), jnp.bfloat16),
            pltpu.VMEM((2 * half, width), jnp.float32),
        ],
        compiler_params=pltpu.CompilerParams(
            dimension_semantics=("arbitrary",), vmem_limit_bytes=20 * 1024 * 1024
        ),
        cost_estimate=pl.CostEstimate(
            flops=12 * half * width * hidden,
            bytes_accessed=6 * width * hidden + 8 * half * width,
            transcendentals=2 * half * hidden,
        ),
        name="expert",
    )(top, low, gate_proj, up_proj, down_proj)


def taps_body(rows_ref, history_ref, taps_ref, mixed_ref, sums_ref, squares_ref, window, taps):
    count, width = rows_ref.shape
    reach = taps_ref.shape[0] - 1
    lead = history_ref.shape[0]
    lanes = window.shape[2]
    tiles = width // lanes
    for tile in range(tiles):
        columns = slice(tile * lanes, (tile + 1) * lanes)
        window[tile, :lead] = history_ref[:, columns].astype(jnp.float32)
        window[tile, lead:] = rows_ref[:, columns].astype(jnp.float32)
        taps[tile, : reach + 1] = taps_ref[:, columns].astype(jnp.float32)
    block = 128
    ones = jnp.ones((8, lanes), jnp.float32)

    def across_lanes(value):
        return lax.dot_general(
            ones,
            value,
            (((1,), (1,)), ((), ())),
            precision=lax.Precision.HIGHEST,
            preferred_element_type=jnp.float32,
        )[0:1]

    @pl.loop(0, count // block)
    def _(step):
        base = step * block

        def one(tile, carry):
            total = jnp.zeros((block, lanes), jnp.float32)
            for offset in range(reach + 1):
                part = window[tile, pl.ds(base + (lead - reach + offset), block), :]
                total = total + part * taps[tile, offset : offset + 1, :]
            at = pl.multiple_of(base, block)
            mixed_ref[tile, pl.ds(at, block), :] = total
            return carry

        lax.fori_loop(0, tiles, one, 0)
        at = pl.multiple_of(base, block)
        parts = [mixed_ref[tile, pl.ds(at, block), :] for tile in range(tiles)]
        sums_ref[pl.ds(step, 1), :] = across_lanes(sum(parts))
        squares_ref[pl.ds(step, 1), :] = across_lanes(sum(part * part for part in parts))


def convolved(rows, history, taps):
    count, width = rows.shape
    lanes = 128
    tiles = width // lanes
    stats = jax.ShapeDtypeStruct((count // 128, 128), jnp.float32)
    return pl.pallas_call(
        taps_body,
        out_shape=[jax.ShapeDtypeStruct((tiles, count, lanes), jnp.float32), stats, stats],
        scratch_shapes=[
            pltpu.VMEM((tiles, count + history.shape[0], lanes), jnp.float32),
            pltpu.VMEM((tiles, 32, lanes), jnp.float32),
        ],
        compiler_params=pltpu.CompilerParams(vmem_limit_bytes=12 * 1024 * 1024),
        cost_estimate=pl.CostEstimate(
            flops=400 * taps.shape[0] * count * width,
            bytes_accessed=6 * count * width,
            transcendentals=0,
        ),
        name="taps",
    )(rows, history, taps)


def pick_body(select_ref, *refs):
    pieces, out_ref, group = refs[:-2], refs[-2], refs[-1]
    own = pieces[0].shape[0]
    for index, piece in enumerate(pieces):
        group[index * own : (index + 1) * own] = piece[...]
    width = group.shape[1]
    wide = 512
    for start in range(0, width, wide):
        columns = slice(start, start + wide)
        rows = dot(select_ref[...], group[:, columns]).astype(jnp.bfloat16)
        out_ref[:, :, columns] = rows.reshape(out_ref.shape[0], out_ref.shape[1], wide)


def picked(select, pieces, share):
    slots, width = select.shape[0], pieces[0].shape[1]
    return pl.pallas_call(
        pick_body,
        out_shape=jax.ShapeDtypeStruct((slots // share, share, width), jnp.bfloat16),
        scratch_shapes=[pltpu.VMEM((select.shape[1], width), jnp.bfloat16)],
        cost_estimate=pl.CostEstimate(
            flops=2 * slots * select.shape[1] * width,
            bytes_accessed=4 * slots * width,
            transcendentals=0,
        ),
        compiler_params=pltpu.CompilerParams(vmem_limit_bytes=10 * 1024 * 1024),
        name="pick",
    )(select, *pieces)


def halves_body(whole_ref, top_ref, low_ref):
    near = whole_ref.shape[0] // 2
    top_ref[...] = whole_ref[:near].reshape(top_ref.shape)
    low_ref[...] = whole_ref[near:].reshape(low_ref.shape)


def halves(whole):
    peers, share, width = whole.shape
    shape = jax.ShapeDtypeStruct((peers * share // 2, width), jnp.bfloat16)
    return pl.pallas_call(halves_body, out_shape=[shape, shape], compiler_params=pltpu.CompilerParams(vmem_limit_bytes=10 * 1024 * 1024), name="halves")(whole)


def close_body(*refs):
    out_ref = refs[-1]
    near = out_ref.shape[0] // 2
    for index in range(2):
        terms = [ref[...].astype(jnp.float32) for ref in refs[3 * index : 3 * index + 3]]
        whole = (terms[0] + terms[1] + terms[2]).astype(jnp.bfloat16)
        out_ref[near * index : near * (index + 1)] = whole.reshape(near, *out_ref.shape[1:])


def closed(top, low, peers):
    rows, width = top[0].shape
    return pl.pallas_call(
        close_body,
        out_shape=jax.ShapeDtypeStruct((peers, 2 * rows // peers, width), jnp.bfloat16),
        compiler_params=pltpu.CompilerParams(vmem_limit_bytes=10 * 1024 * 1024),
        name="close",
    )(*top, *low)


def mix_body(returned_ref, *refs):
    terms, outs = refs[:3], refs[3:]
    slots = returned_ref.shape[0] * returned_ref.shape[1]
    width = returned_ref.shape[2]
    own = outs[0].shape[0]
    wide = 512
    for start in range(0, width, wide):
        columns = slice(start, start + wide)
        rows = returned_ref[:, :, columns].reshape(slots, wide)
        total = sum(
            lax.dot_general(
                ref[...], rows, (((0,), (0,)), ((), ())), preferred_element_type=jnp.float32
            )
            for ref in terms
        ).astype(jnp.bfloat16)
        for index, out in enumerate(outs):
            out[:, columns] = total[index * own : (index + 1) * own]


def mixed_in(returned, terms, pieces):
    width = returned.shape[2]
    own = jax.ShapeDtypeStruct((terms[0].shape[1] // pieces, width), jnp.bfloat16)
    return pl.pallas_call(mix_body, out_shape=[own] * pieces, compiler_params=pltpu.CompilerParams(vmem_limit_bytes=10 * 1024 * 1024), name="mix")(returned, *terms)


def local(
    conv_input,
    conv_kernel,
    norm_gain,
    norm_shift,
    conv_proj,
    moe_input,
    moe_gain,
    routes,
    route_weights,
    gate_proj,
    up_proj,
    down_proj,
):
    tp_count = lax.axis_size("tp")
    ep_count = lax.axis_size("ep")
    tp_index = lax.axis_index("tp")
    group_rows, top_count = routes.shape
    own_rows, _ = moe_input.shape
    capacity = 2 * top_count * group_rows // ep_count
    share = capacity // tp_count
    slots = ep_count * share

    moe_float = moe_input.astype(jnp.float32)
    normed = (
        moe_float
        * lax.rsqrt(jnp.mean(moe_float * moe_float, axis=1, keepdims=True) + 1e-06)
        * moe_gain
    ).astype(jnp.bfloat16)
    normed, conv_input = tied(normed, conv_input)
    pieces = (normed, turned(normed, -1), turned(normed, 2), turned(normed, 1))
    history = shifted(conv_input[conv_input.shape[0] - 32 :], "ep", 1)

    experts = jnp.arange(ep_count, dtype=jnp.int32)
    hits = routes.T[:, None, :] == experts[None, :, None]
    chosen = jnp.any(hits, axis=0)
    before = (
        lax.broadcasted_iota(jnp.int32, (group_rows, group_rows), 0)
        < lax.broadcasted_iota(jnp.int32, (group_rows, group_rows), 1)
    ).astype(jnp.bfloat16)
    rank = dot(chosen.astype(jnp.bfloat16), before).astype(jnp.int32)
    local_rank = jnp.where(chosen, rank - tp_index * share, -1)

    def from_here(table):
        return lax.dynamic_slice_in_dim(
            jnp.concatenate([table, table], axis=1), tp_index * own_rows, group_rows, axis=1
        )

    select = from_here(local_rank)[:, None, :] == jnp.arange(share, dtype=jnp.int32)[None, :, None]
    select = select.astype(jnp.bfloat16).reshape(slots, group_rows)
    *pieces, select, history = tied(*pieces, select, history)

    rows = picked(select, pieces, share)
    rows, routes, route_weights, conv_input = tied(rows, routes, route_weights, conv_input)
    landed = lax.all_to_all(rows, "ep", split_axis=0, concat_axis=0, tiled=True)

    local_rows, local_width = conv_input.shape
    mixed, *stats = convolved(conv_input, history, conv_kernel)
    full_width = local_width * tp_count
    sums, squares = lax.psum(tuple(stats), "tp")
    center = sums / full_width
    spread = jnp.maximum(squares / full_width - center * center, 0.0)
    factor = lax.rsqrt(spread + 1e-05)
    mixed = jnp.concatenate(list(mixed), axis=1)
    scaled = (mixed - center.reshape(-1, 1)) * factor.reshape(-1, 1) * norm_gain + norm_shift
    activated = jax.nn.silu(scaled).astype(jnp.bfloat16)
    half = local_rows // (2 * tp_count)

    def projected(rows, step, offset):
        start = lax.rem(tp_index + step, tp_count) * (2 * half) + offset
        part = lax.dynamic_slice_in_dim(rows, start, half, axis=0)
        return dot(part, conv_proj).astype(jnp.bfloat16)

    conv_top, conv_low = projected(activated, 2, 0), projected(activated, 2, half)
    conv_top, conv_low = turned(conv_top, 1), turned(conv_low, -1)
    landed, activated, routes, route_weights = tied(landed, activated, routes, route_weights)

    own = halves(landed)
    left_top, right_low = turned(own[0], 1), turned(own[1], -1)
    left_low, right_top = turned(own[1], 1), turned(own[0], -1)
    matrices = (gate_proj, up_proj, down_proj)
    own = list(expert(*own, *matrices))
    left_top, right_low, own[0] = tied(left_top, right_low, own[0])
    far_top, far_low = turned(left_top, 1), turned(right_low, -1)

    activated, routes, route_weights, left_top = tied(activated, routes, route_weights, left_top)
    hits = routes.T[:, None, :] == experts[None, :, None]
    weight_of = jnp.sum(jnp.where(hits, route_weights.T[:, None, :], 0.0), axis=0)
    weights = jnp.repeat(from_here(weight_of), share, axis=0) * select.astype(jnp.float32)
    terms = in_three(weights)
    conv_right = [projected(activated, 1, offset) for offset in (0, half)]
    conv_left = [projected(activated, 3, offset) for offset in (0, half)]
    conv_own = [projected(activated, 0, offset) for offset in (0, half)]

    left_top, right_low = expert(left_top, right_low, *matrices)
    flat = tied(left_top, right_low, right_top, left_low, *conv_right, *conv_left, *conv_own, *terms)
    left_top, right_low, right_top, left_low = flat[:4]
    conv_right, conv_left, conv_own, terms = flat[4:6], flat[6:8], flat[8:10], flat[10:]
    early_left, early_right = turned(right_low, 1), turned(left_top, -1)
    right_top, left_low = expert(right_top, left_low, *matrices)
    far_top, far_low, right_top, left_low = tied(far_top, far_low, right_top, left_low)
    far_top, far_low = expert(far_top, far_low, *matrices)
    via_left, via_right = turned(far_top, 1), turned(far_low, -1)
    conv_right = (rounded_sum(conv_right[0], conv_top), conv_right[1])
    conv_left = (conv_left[0], rounded_sum(conv_left[1], conv_low))
    via_left, via_right, *conv_sums = tied(via_left, via_right, conv_right[0], conv_left[1])
    conv_right, conv_left = (conv_sums[0], conv_right[1]), (conv_left[0], conv_sums[1])
    late_left = turned(rounded_sum(right_top, via_left), 1)
    late_right = turned(rounded_sum(left_low, via_right), -1)
    totals = closed(
        (own[0], late_left, early_right), (own[1], early_left, late_right), ep_count
    )

    flat = tied(totals, *conv_right, *conv_left)
    totals, conv_right, conv_left = flat[0], flat[1:3], flat[3:5]
    returned = lax.all_to_all(totals, "ep", split_axis=0, concat_axis=0, tiled=True)
    conv_top = [turned(conv_right[0], 1), turned(conv_left[0], -1)]
    conv_low = [turned(conv_right[1], 1), turned(conv_left[1], -1)]
    own, right, far, left = mixed_in(returned, terms, tp_count)
    arrived = [turned(far, 2), turned(right, 1), turned(left, -1)]
    conv_out = jnp.concatenate(
        [rounded_sum(conv_own[0], *conv_top), rounded_sum(conv_own[1], *conv_low)], axis=0
    )
    *arrived, conv_out = tied(*arrived, conv_out)
    moe_out = rounded_sum(own, *arrived)
    return (conv_out, moe_out)


def solution(mesh):
    placed = (
        P("ep", "tp"),
        P(None, "tp"),
        P("tp"),
        P("tp"),
        P("tp", None),
        P(("ep", "tp"), None),
        P(),
        P("ep", None),
        P("ep", None),
        P("ep", None, "tp"),
        P("ep", None, "tp"),
        P("ep", "tp", None),
    )
    return jax.shard_map(
        local,
        mesh=mesh,
        in_specs=placed,
        out_specs=(P(("ep", "tp"), None), P(("ep", "tp"), None)),
        check_vma=False,
    )
```

```python
import jax
import jax.numpy as jnp
from jax import lax
from jax.experimental import pallas as pl
from jax.experimental.pallas import tpu as pltpu
from jax.sharding import PartitionSpec as P


def shifted(value, axis, steps):
    count = lax.axis_size(axis)
    leading, last = (max(0, -steps), min(count, count - steps))
    return lax.ppermute(value, axis, [(source, source + steps) for source in range(leading, last)])


def turned(value, steps):
    count = lax.axis_size("tp")
    return lax.ppermute(value, "tp", [(i, (i + steps) % count) for i in range(count)])


def dot(lhs, rhs):
    return jnp.dot(lhs, rhs, preferred_element_type=jnp.float32)


def in_three(value):
    high = lax.reduce_precision(value, 8, 7)
    rest = value - high
    middle = lax.reduce_precision(rest, 8, 7)
    low = rest - middle
    return [term.astype(jnp.bfloat16) for term in (high, middle, low)]


def tied(*values):
    return lax.optimization_barrier(values)


def rounded_sum(*values):
    return sum(value.astype(jnp.float32) for value in values).astype(jnp.bfloat16)


def expert_body(top_ref, low_ref, gate_ref, up_ref, down_ref, top_out, low_out, rows, total):
    step = pl.program_id(0)
    half = top_ref.shape[0]

    @pl.when(step == 0)
    def _():
        rows[:half] = top_ref[...]
        rows[half:] = low_ref[...]

    gated = dot(rows[...], gate_ref[0])
    raised = dot(rows[...], up_ref[0])
    hidden = (gated / (1.0 + jnp.exp(-gated)) * raised).astype(jnp.bfloat16)
    added = dot(hidden, down_ref[0])

    @pl.when(step == 0)
    def _():
        total[...] = added

    @pl.when(step == pl.num_programs(0) - 1)
    def _():
        top_out[...] = (total[:half] + added[:half]).astype(jnp.bfloat16)
        low_out[...] = (total[half:] + added[half:]).astype(jnp.bfloat16)


def expert(top, low, gate_proj, up_proj, down_proj):
    half, width = top.shape
    hidden = gate_proj.shape[2]
    steps = 2
    tile = hidden // steps
    block = pl.BlockSpec((half, width), lambda i: (0, 0))
    shape = jax.ShapeDtypeStruct((half, width), jnp.bfloat16)
    return pl.pallas_call(
        expert_body,
        grid=(steps,),
        in_specs=[
            block,
            block,
            pl.BlockSpec((1, width, tile), lambda i: (0, 0, i)),
            pl.BlockSpec((1, width, tile), lambda i: (0, 0, i)),
            pl.BlockSpec((1, tile, width), lambda i: (0, i, 0)),
        ],
        out_specs=[block, block],
        out_shape=[shape, shape],
        scratch_shapes=[
            pltpu.VMEM((2 * half, width), jnp.bfloat16),
            pltpu.VMEM((2 * half, width), jnp.float32),
        ],
        compiler_params=pltpu.CompilerParams(
            dimension_semantics=("arbitrary",), vmem_limit_bytes=20 * 1024 * 1024
        ),
        cost_estimate=pl.CostEstimate(
            flops=12 * half * width * hidden,
            bytes_accessed=6 * width * hidden + 8 * half * width,
            transcendentals=2 * half * hidden,
        ),
        name="expert",
    )(top, low, gate_proj, up_proj, down_proj)


def taps_body(rows_ref, history_ref, taps_ref, mixed_ref, sums_ref, squares_ref, window, taps):
    count, width = rows_ref.shape
    reach = taps_ref.shape[0] - 1
    lead = history_ref.shape[0]
    lanes = window.shape[2]
    tiles = width // lanes
    for tile in range(tiles):
        columns = slice(tile * lanes, (tile + 1) * lanes)
        window[tile, :lead] = history_ref[:, columns].astype(jnp.float32)
        window[tile, lead:] = rows_ref[:, columns].astype(jnp.float32)
        taps[tile, : reach + 1] = taps_ref[:, columns].astype(jnp.float32)
    block = 128
    ones = jnp.ones((8, lanes), jnp.float32)

    def across_lanes(value):
        return lax.dot_general(
            ones,
            value,
            (((1,), (1,)), ((), ())),
            precision=lax.Precision.HIGHEST,
            preferred_element_type=jnp.float32,
        )[0:1]

    @pl.loop(0, count // block)
    def _(step):
        base = step * block

        def one(tile, carry):
            total = jnp.zeros((block, lanes), jnp.float32)
            for offset in range(reach + 1):
                part = window[tile, pl.ds(base + (lead - reach + offset), block), :]
                total = total + part * taps[tile, offset : offset + 1, :]
            at = pl.multiple_of(base, block)
            mixed_ref[tile, pl.ds(at, block), :] = total
            return carry

        lax.fori_loop(0, tiles, one, 0)
        at = pl.multiple_of(base, block)
        parts = [mixed_ref[tile, pl.ds(at, block), :] for tile in range(tiles)]
        sums_ref[pl.ds(step, 1), :] = across_lanes(sum(parts))
        squares_ref[pl.ds(step, 1), :] = across_lanes(sum(part * part for part in parts))


def convolved(rows, history, taps):
    count, width = rows.shape
    lanes = 128
    tiles = width // lanes
    stats = jax.ShapeDtypeStruct((count // 128, 128), jnp.float32)
    return pl.pallas_call(
        taps_body,
        out_shape=[jax.ShapeDtypeStruct((tiles, count, lanes), jnp.float32), stats, stats],
        scratch_shapes=[
            pltpu.VMEM((tiles, count + history.shape[0], lanes), jnp.float32),
            pltpu.VMEM((tiles, 32, lanes), jnp.float32),
        ],
        compiler_params=pltpu.CompilerParams(vmem_limit_bytes=12 * 1024 * 1024),
        cost_estimate=pl.CostEstimate(
            flops=400 * taps.shape[0] * count * width,
            bytes_accessed=6 * count * width,
            transcendentals=0,
        ),
        name="taps",
    )(rows, history, taps)


def norm_body(rows_ref, gain_ref, out_ref):
    rows = rows_ref[...].astype(jnp.float32)
    mean = jnp.mean(rows * rows, axis=1, keepdims=True)
    out_ref[...] = (rows * lax.rsqrt(mean + 1e-06) * gain_ref[...]).astype(jnp.bfloat16)


def normalized(rows, gain):
    return pl.pallas_call(
        norm_body,
        out_shape=jax.ShapeDtypeStruct(rows.shape, jnp.bfloat16),
        compiler_params=pltpu.CompilerParams(vmem_limit_bytes=10 * 1024 * 1024),
        name="norm",
    )(rows, gain[None])


def pick_body(select_ref, *refs):
    pieces, out_ref, group = refs[:-2], refs[-2], refs[-1]
    own = pieces[0].shape[0]
    for index, piece in enumerate(pieces):
        group[index * own : (index + 1) * own] = piece[...]
    width = group.shape[1]
    wide = 512
    for start in range(0, width, wide):
        columns = slice(start, start + wide)
        rows = dot(select_ref[...], group[:, columns]).astype(jnp.bfloat16)
        out_ref[:, :, columns] = rows.reshape(out_ref.shape[0], out_ref.shape[1], wide)


def picked(select, pieces, share):
    slots, width = select.shape[0], pieces[0].shape[1]
    return pl.pallas_call(
        pick_body,
        out_shape=jax.ShapeDtypeStruct((slots // share, share, width), jnp.bfloat16),
        scratch_shapes=[pltpu.VMEM((select.shape[1], width), jnp.bfloat16)],
        cost_estimate=pl.CostEstimate(
            flops=2 * slots * select.shape[1] * width,
            bytes_accessed=4 * slots * width,
            transcendentals=0,
        ),
        compiler_params=pltpu.CompilerParams(vmem_limit_bytes=10 * 1024 * 1024),
        name="pick",
    )(select, *pieces)


def halves_body(whole_ref, top_ref, low_ref):
    near = whole_ref.shape[0] // 2
    top_ref[...] = whole_ref[:near].reshape(top_ref.shape)
    low_ref[...] = whole_ref[near:].reshape(low_ref.shape)


def halves(whole):
    peers, share, width = whole.shape
    shape = jax.ShapeDtypeStruct((peers * share // 2, width), jnp.bfloat16)
    return pl.pallas_call(halves_body, out_shape=[shape, shape], compiler_params=pltpu.CompilerParams(vmem_limit_bytes=10 * 1024 * 1024), name="halves")(whole)


def close_body(*refs):
    out_ref = refs[-1]
    near = out_ref.shape[0] // 2
    for index in range(2):
        terms = [ref[...].astype(jnp.float32) for ref in refs[3 * index : 3 * index + 3]]
        whole = (terms[0] + terms[1] + terms[2]).astype(jnp.bfloat16)
        out_ref[near * index : near * (index + 1)] = whole.reshape(near, *out_ref.shape[1:])


def closed(top, low, peers):
    rows, width = top[0].shape
    return pl.pallas_call(
        close_body,
        out_shape=jax.ShapeDtypeStruct((peers, 2 * rows // peers, width), jnp.bfloat16),
        compiler_params=pltpu.CompilerParams(vmem_limit_bytes=10 * 1024 * 1024),
        name="close",
    )(*top, *low)


def mix_body(returned_ref, *refs):
    terms, outs = refs[:3], refs[3:]
    slots = returned_ref.shape[0] * returned_ref.shape[1]
    width = returned_ref.shape[2]
    own = outs[0].shape[0]
    wide = 512
    for start in range(0, width, wide):
        columns = slice(start, start + wide)
        rows = returned_ref[:, :, columns].reshape(slots, wide)
        total = sum(
            lax.dot_general(
                ref[...], rows, (((0,), (0,)), ((), ())), preferred_element_type=jnp.float32
            )
            for ref in terms
        ).astype(jnp.bfloat16)
        for index, out in enumerate(outs):
            out[:, columns] = total[index * own : (index + 1) * own]


def mixed_in(returned, terms, pieces):
    width = returned.shape[2]
    own = jax.ShapeDtypeStruct((terms[0].shape[1] // pieces, width), jnp.bfloat16)
    return pl.pallas_call(mix_body, out_shape=[own] * pieces, compiler_params=pltpu.CompilerParams(vmem_limit_bytes=10 * 1024 * 1024), name="mix")(returned, *terms)


def local(
    conv_input,
    conv_kernel,
    norm_gain,
    norm_shift,
    conv_proj,
    moe_input,
    moe_gain,
    routes,
    route_weights,
    gate_proj,
    up_proj,
    down_proj,
):
    tp_count = lax.axis_size("tp")
    ep_count = lax.axis_size("ep")
    tp_index = lax.axis_index("tp")
    group_rows, top_count = routes.shape
    own_rows, _ = moe_input.shape
    capacity = 2 * top_count * group_rows // ep_count
    share = capacity // tp_count
    slots = ep_count * share

    normed = normalized(moe_input, moe_gain)
    normed, conv_input = tied(normed, conv_input)
    pieces = (normed, turned(normed, -1), turned(normed, 2), turned(normed, 1))
    history = shifted(conv_input[conv_input.shape[0] - 32 :], "ep", 1)

    experts = jnp.arange(ep_count, dtype=jnp.int32)
    hits = routes.T[:, None, :] == experts[None, :, None]
    chosen = jnp.any(hits, axis=0)
    before = (
        lax.broadcasted_iota(jnp.int32, (group_rows, group_rows), 0)
        < lax.broadcasted_iota(jnp.int32, (group_rows, group_rows), 1)
    ).astype(jnp.bfloat16)
    rank = dot(chosen.astype(jnp.bfloat16), before).astype(jnp.int32)
    local_rank = jnp.where(chosen, rank - tp_index * share, -1)

    def from_here(table):
        return lax.dynamic_slice_in_dim(
            jnp.concatenate([table, table], axis=1), tp_index * own_rows, group_rows, axis=1
        )

    select = from_here(local_rank)[:, None, :] == jnp.arange(share, dtype=jnp.int32)[None, :, None]
    select = select.astype(jnp.bfloat16).reshape(slots, group_rows)
    *pieces, select, history = tied(*pieces, select, history)

    rows = picked(select, pieces, share)
    rows, routes, route_weights, conv_input = tied(rows, routes, route_weights, conv_input)
    landed = lax.all_to_all(rows, "ep", split_axis=0, concat_axis=0, tiled=True)

    local_rows, local_width = conv_input.shape
    mixed, *stats = convolved(conv_input, history, conv_kernel)
    full_width = local_width * tp_count
    stats = jnp.concatenate(stats, axis=0)
    for pairs in (((0, 1), (2, 3)), ((0, 3), (1, 2))):
        swapped = [*pairs, *((to, source) for source, to in pairs)]
        stats = stats + lax.ppermute(stats, "tp", swapped)
    sums, squares = jnp.split(stats, 2, axis=0)
    center = sums / full_width
    spread = jnp.maximum(squares / full_width - center * center, 0.0)
    factor = lax.rsqrt(spread + 1e-05)
    mixed = jnp.concatenate(list(mixed), axis=1)
    scaled = (mixed - center.reshape(-1, 1)) * factor.reshape(-1, 1) * norm_gain + norm_shift
    activated = jax.nn.silu(scaled).astype(jnp.bfloat16)
    half = local_rows // (2 * tp_count)

    def projected(rows, step, offset):
        start = lax.rem(tp_index + step, tp_count) * (2 * half) + offset
        part = lax.dynamic_slice_in_dim(rows, start, half, axis=0)
        return dot(part, conv_proj).astype(jnp.bfloat16)

    conv_top, conv_low = projected(activated, 2, 0), projected(activated, 2, half)
    conv_top, conv_low = turned(conv_top, 1), turned(conv_low, -1)
    landed, activated, routes, route_weights = tied(landed, activated, routes, route_weights)

    own = halves(landed)
    left_top, right_low = turned(own[0], 1), turned(own[1], -1)
    left_low, right_top = turned(own[1], 1), turned(own[0], -1)
    matrices = (gate_proj, up_proj, down_proj)
    own = list(expert(*own, *matrices))
    left_top, right_low, own[0] = tied(left_top, right_low, own[0])
    far_top, far_low = turned(left_top, 1), turned(right_low, -1)

    activated, routes, route_weights, left_top = tied(activated, routes, route_weights, left_top)
    hits = routes.T[:, None, :] == experts[None, :, None]
    weight_of = jnp.sum(jnp.where(hits, route_weights.T[:, None, :], 0.0), axis=0)
    weights = jnp.repeat(from_here(weight_of), share, axis=0) * select.astype(jnp.float32)
    terms = in_three(weights)
    conv_right = [projected(activated, 1, offset) for offset in (0, half)]
    conv_left = [projected(activated, 3, offset) for offset in (0, half)]
    conv_own = [projected(activated, 0, offset) for offset in (0, half)]

    left_top, right_low = expert(left_top, right_low, *matrices)
    flat = tied(left_top, right_low, right_top, left_low, *conv_right, *conv_left, *conv_own, *terms)
    left_top, right_low, right_top, left_low = flat[:4]
    conv_right, conv_left, conv_own, terms = flat[4:6], flat[6:8], flat[8:10], flat[10:]
    early_left, early_right = turned(right_low, 1), turned(left_top, -1)
    right_top, left_low = expert(right_top, left_low, *matrices)
    far_top, far_low, right_top, left_low = tied(far_top, far_low, right_top, left_low)
    far_top, far_low = expert(far_top, far_low, *matrices)
    via_left, via_right = turned(far_top, 1), turned(far_low, -1)
    conv_right = (rounded_sum(conv_right[0], conv_top), conv_right[1])
    conv_left = (conv_left[0], rounded_sum(conv_left[1], conv_low))
    via_left, via_right, *conv_sums = tied(via_left, via_right, conv_right[0], conv_left[1])
    conv_right, conv_left = (conv_sums[0], conv_right[1]), (conv_left[0], conv_sums[1])
    late_left = turned(rounded_sum(right_top, via_left), 1)
    late_right = turned(rounded_sum(left_low, via_right), -1)
    totals = closed(
        (own[0], late_left, early_right), (own[1], early_left, late_right), ep_count
    )

    flat = tied(totals, *conv_right, *conv_left)
    totals, conv_right, conv_left = flat[0], flat[1:3], flat[3:5]
    returned = lax.all_to_all(totals, "ep", split_axis=0, concat_axis=0, tiled=True)
    conv_top = [turned(conv_right[0], 1), turned(conv_left[0], -1)]
    conv_low = [turned(conv_right[1], 1), turned(conv_left[1], -1)]
    own, right, far, left = mixed_in(returned, terms, tp_count)
    arrived = [turned(far, 2), turned(right, 1), turned(left, -1)]
    conv_out = jnp.concatenate(
        [rounded_sum(conv_own[0], *conv_top), rounded_sum(conv_own[1], *conv_low)], axis=0
    )
    *arrived, conv_out = tied(*arrived, conv_out)
    moe_out = rounded_sum(own, *arrived)
    return (conv_out, moe_out)


def solution(mesh):
    placed = (
        P("ep", "tp"),
        P(None, "tp"),
        P("tp"),
        P("tp"),
        P("tp", None),
        P(("ep", "tp"), None),
        P(),
        P("ep", None),
        P("ep", None),
        P("ep", None, "tp"),
        P("ep", None, "tp"),
        P("ep", "tp", None),
    )
    return jax.shard_map(
        local,
        mesh=mesh,
        in_specs=placed,
        out_specs=(P(("ep", "tp"), None), P(("ep", "tp"), None)),
        check_vma=False,
    )
```
